32 devices in a mesh: sp: 4 (over y, x), tp: 8 (over z, core).
Axes of the slice: x: 2, y: 2, z: 4, core: 2. Of those that a mesh axis runs over, the one named last changes fastest.
Arguments:
- prompt: bfloat16 [2, 8, 2, 4, 128, 2048], P(None, 'tp', None, 'sp'), may hold values from -60 to 60
- new_token: bfloat16 [2, 2048], replicated, may hold values from -20 to 20
- query_proj_matrix: bfloat16 [2048, 1024], P(None, 'tp'), may hold values from -1 to 1
- key_weight: bfloat16 [2048, 1024], P(None, 'tp'), may hold values from -1 to 1
- value_weight: bfloat16 [2048, 1024], P(None, 'tp'), may hold values from -0.125 to 0.125
- map_balance: float32 [8], replicated, may hold values from 0.3 to 0.8
- head_gain: float32 [128], replicated, may hold values from 0.1 to 1.9
Outputs:
- key_cache: bfloat16 [4, 8, 512, 1024], P('sp', 'tp')
- value_cache: bfloat16 [4, 8, 512, 1024], P('sp', 'tp')
- read: float32 [2, 1024], replicated
The draws below stay inside these ranges and needn't reach their ends.
All inputs are finite; a program needn't handle non-finite values.
Results may differ from the reference program's by a relative error of at most 0.004.
The reference program's roundings to bfloat16 on the way (of `queries`) count: a program that leaves them out, or rounds other values in their place, can miss the bound.
Values may be sent and summed in bfloat16 or wider, within the bound.
No kernel may reach another device: no remote copies, remote signals or barrier semaphores. Data moves between devices by JAX's collectives and lax.ppermute only.
A program may use at most 64 MiB of HBM per device.

```python
import math
import jax
import jax.numpy as jnp
from jax import lax

D = 2048
HEADS = 8
MAP_HEAD_SIZE = 64
VD = 128
SEQS = 2
KW = 1024
VW = 1024
GROUP = 2
SUB = 128
TILES = 8
SPAN = 512
LEN = 8192
N_SP = 4


def shared_query(key):
    base = jax.random.normal(jax.random.fold_in(key, 11), (D, KW), jnp.float32)
    return jnp.clip(base, -6.0, 6.0) / math.sqrt(D)


def shared_new(key):
    base = jnp.clip(jax.random.normal(jax.random.fold_in(key, 13), (SEQS, D), jnp.float32), -6.0, 6.0) * 1.3
    return base


def draw_query_proj_matrix(key, part):
    return shared_query(key).astype(jnp.bfloat16)


def draw_key_weight(key, part):
    base = jax.random.normal(jax.random.fold_in(key, 12), (D, KW), jnp.float32)
    own = jnp.clip(base, -6.0, 6.0) / math.sqrt(D)
    matrix = own
    return matrix.astype(jnp.bfloat16)


def draw_new_token(key, part):
    return shared_new(key).astype(jnp.bfloat16)


def draw_prompt(key, part):
    base = jax.random.normal(jax.random.fold_in(key, 14), (SEQS, LEN, D), jnp.float32)
    base = jnp.clip(base, -6.0, 6.0) * 1.3
    return base.reshape(SEQS, TILES, GROUP, N_SP, SUB, D).astype(jnp.bfloat16)


def block_levels(rng, shape, pieces, smallest, top_value):
    loudness = 1.0
    for axis_at, blocks in pieces:
        draws = jax.random.uniform(jax.random.fold_in(jax.random.fold_in(rng, 6), axis_at), (blocks,), jnp.float32, smallest / len(pieces), top_value / len(pieces))
        loudness = loudness * jnp.repeat(jnp.exp(draws), shape[axis_at] // blocks).reshape((-1,) + (1,) * (len(shape) - 1 - axis_at))
    return loudness


def normal_values(stream_key, dims, spread, reach, pieces=(), held_as=jnp.bfloat16):
    result = spread * jax.random.normal(stream_key, dims, jnp.float32)
    if pieces:
        result = result * block_levels(stream_key, dims, pieces, -0.22, 0.18)
    return jnp.clip(result, -reach, reach).astype(held_as)


def setup_inputs(seed: int = 0) -> dict:
    splits = jax.random.split(jax.random.key(seed), 8)
    return {
        "prompt": draw_prompt(jax.random.fold_in(splits[7], 71), 0),
        "new_token": draw_new_token(jax.random.fold_in(splits[7], 71), 0),
        "query_proj_matrix": draw_query_proj_matrix(jax.random.fold_in(splits[7], 71), 0),
        "key_weight": draw_key_weight(jax.random.fold_in(splits[7], 71), 0),
        "value_weight": normal_values(splits[4], (D, VW), D ** -0.5, 0.125, ((1, 8),)),
        "map_balance": jnp.clip(jax.random.uniform(splits[5], (HEADS,), jnp.float32, 0.3, 0.8), 0.3, 0.8),
        "head_gain": jnp.clip(1.0 + 0.18 * jax.random.normal(splits[6], (VD,), jnp.float32), 0.1, 1.9),
    }


norm_eps = 1e-06

def project(inputs, weight_matrix):
    return jnp.dot(inputs, weight_matrix, preferred_element_type=jnp.float32).astype(jnp.bfloat16)

def relayout(rows, width):
    shaped = rows.reshape(SEQS, TILES, GROUP, SPAN, width)
    return jnp.transpose(shaped, (0, 2, 1, 3, 4)).reshape(SEQS * GROUP, TILES, SPAN, width)

def reference(prompt, new_token, query_proj_matrix, key_weight, value_weight, map_balance, head_gain):

    def cache_rows(sequence):
        flat_rows = sequence.reshape(LEN, D)
        return (project(flat_rows, key_weight), project(flat_rows, value_weight))
    flat_keys, flat_values = lax.map(cache_rows, prompt)
    queries = project(new_token, query_proj_matrix)
    new_keys = project(new_token, key_weight)
    new_values = project(new_token, value_weight)

    def read_one(inputs):
        seq_keys, seq_values, own_query, own_key, own_value = inputs
        every_key_row = jnp.concatenate([seq_keys, own_key[None, :]], axis=0)
        every_key_row = every_key_row.astype(jnp.float32).reshape(LEN + 1, HEADS, 2, MAP_HEAD_SIZE)
        all_values = jnp.concatenate([seq_values, own_value[None, :]], axis=0)
        all_values = all_values.astype(jnp.float32).reshape(LEN + 1, HEADS, VD)
        query_matrix_rows = own_query.astype(jnp.float32).reshape(HEADS, 2, MAP_HEAD_SIZE)
        logit_scores = jnp.einsum('rkx,vrkx->rkv', query_matrix_rows, every_key_row) * MAP_HEAD_SIZE ** (-0.5)
        probs = jax.nn.softmax(logit_scores, axis=-1)
        heads_out = jnp.einsum('hmj,jhe->hme', probs, all_values)
        blended = heads_out[:, 0] - map_balance[:, None] * heads_out[:, 1]
        normed = blended * lax.rsqrt(lax.optimization_barrier(jnp.mean(blended * blended, axis=-1, keepdims=True)) + norm_eps) * head_gain
        return normed.reshape(HEADS * VD)
    read = lax.map(read_one, (flat_keys, flat_values, queries, new_keys, new_values))
    return (relayout(flat_keys, KW), relayout(flat_values, VW), read)
```

```python
import jax
import jax.numpy as jnp
from jax import lax
from jax.sharding import PartitionSpec as P

HEADS = 8
MAP_HEAD_SIZE = 64
VD = 128


norm_eps = 1e-06


def two_parts(values):
    high = lax.reduce_precision(values, 8, 7)
    return high.astype(jnp.bfloat16), (values - high).astype(jnp.bfloat16)


def project(source, weight):
    return jnp.dot(source, weight, preferred_element_type=jnp.float32).astype(jnp.bfloat16)


def joined(peak, totals, weighted, axis):
    top = jnp.max(peak, axis=axis, keepdims=True)
    factor = jnp.exp(peak - top)
    return (
        jnp.squeeze(top, axis),
        jnp.sum(totals * factor, axis=axis),
        jnp.sum(weighted * factor[..., None], axis=axis),
    )


def packed(peak, totals, weighted):
    lanes = peak.shape + (VD // 2,)
    return jnp.concatenate(
        [
            weighted,
            jnp.broadcast_to(peak[..., None], lanes),
            jnp.broadcast_to(totals[..., None], lanes),
        ],
        axis=-1,
    )


def unpacked(state):
    width = state.shape[-1] - VD
    return state[..., width], state[..., width + VD // 2], state[..., :width]


def own_read(keys, rows, queries, value_weight):
    tp_count = lax.axis_size("tp")
    map_count = 2 * HEADS
    key_width = keys.shape[1]
    of_map = jnp.arange(key_width) // MAP_HEAD_SIZE == jnp.arange(map_count)[:, None]
    spread = jnp.where(of_map, queries[None, :], jnp.zeros((), queries.dtype))
    scores = lax.dot_general(
        spread, keys, (((1,), (1,)), ((), ())), preferred_element_type=jnp.float32
    ) * MAP_HEAD_SIZE ** (-0.5)
    peak = jnp.max(scores, axis=-1)
    weights_exp = jnp.exp(scores - peak[:, None])
    totals = jnp.sum(weights_exp, axis=-1)
    high, low = two_parts(weights_exp)
    mixed = jnp.dot(
        jnp.concatenate([high, low]), rows, preferred_element_type=jnp.float32
    )
    mixed = mixed[:map_count] + mixed[map_count:]
    state = packed(peak, totals, mixed)
    width = value_weight.shape[1]
    heads_here = max(1, width // VD)
    repeats = max(1, VD // width)
    state = state.reshape(HEADS // heads_here, 1, heads_here * 2, state.shape[-1])
    state = jnp.broadcast_to(state, (state.shape[0], repeats) + state.shape[2:])
    state = state.reshape((tp_count,) + state.shape[2:])
    state = lax.all_to_all(state, "tp", 0, 0, tiled=True)
    peak, totals, mixed = joined(*unpacked(state), 0)
    mixed = mixed.reshape(heads_here, 2, -1)
    head_weight = value_weight.reshape(value_weight.shape[0], heads_here, width // heads_here)
    high, low = two_parts(mixed)
    weighted = jnp.einsum(
        "hmd,dhe->hme",
        jnp.concatenate([high, low], axis=1),
        head_weight,
        preferred_element_type=jnp.float32,
    )
    weighted = weighted[:, :2] + weighted[:, 2:]
    return peak, totals, weighted.reshape(heads_here * 2, -1)


def shards(prompt, new_token, query_proj_matrix, key_weight, value_weight, map_balance, head_gain):
    seq_count, _, span_count, _, piece_rows, model_width = prompt.shape
    tp_count = lax.axis_size("tp")
    slot_count = seq_count * span_count
    key_piece = lax.all_gather(key_weight, "tp", axis=1, tiled=True)
    key_width = key_piece.shape[1]
    value_piece = lax.all_gather(value_weight, "tp", axis=1, tiled=True)
    value_width = value_piece.shape[1]
    rows = lax.all_to_all(
        prompt.reshape(slot_count, piece_rows, model_width),
        "sp",
        split_axis=0,
        concat_axis=1,
        tiled=True,
    )
    rows = rows.reshape(-1, model_width)
    own_columns = jnp.stack(
        [project(new_token, w) for w in (query_proj_matrix, key_weight, value_weight)]
    )
    queries, new_keys, new_values = lax.all_gather(own_columns, "tp", axis=2, tiled=True)
    keys = project(rows, key_piece)
    own_seq = lax.axis_index("sp") // span_count
    peak, totals, weighted = own_read(
        keys, rows, lax.dynamic_index_in_dim(queries, own_seq, 0, False), value_weight
    )
    state = lax.all_gather(packed(peak, totals, weighted), "sp")
    state = state.reshape((seq_count, span_count) + state.shape[1:])
    peak, totals, weighted = joined(*unpacked(state), 1)
    state = lax.all_gather(packed(peak, totals, weighted), "tp")
    peak, totals, weighted = unpacked(state)
    heads_here = weighted.shape[2] // 2
    groups = HEADS // heads_here
    repeats = tp_count // groups
    peak, totals = (
        jnp.swapaxes(
            a.reshape(groups, repeats, seq_count, heads_here, 2)[:, 0], 0, 1
        ).reshape(seq_count, HEADS, 2)
        for a in (peak, totals)
    )
    weighted = weighted.reshape(groups, repeats, seq_count, heads_here, 2, -1)
    weighted = jnp.transpose(weighted, (2, 0, 3, 4, 1, 5)).reshape(seq_count, HEADS, 2, VD)
    own_score = jnp.sum(
        (queries.astype(jnp.float32) * new_keys.astype(jnp.float32)).reshape(
            seq_count, HEADS, 2, MAP_HEAD_SIZE
        ),
        axis=-1,
    ) * MAP_HEAD_SIZE ** (-0.5)
    own_values = new_values.astype(jnp.float32).reshape(seq_count, HEADS, 1, VD)
    top = jnp.maximum(peak, own_score)
    cached_factor = jnp.exp(peak - top)
    own_factor = jnp.exp(own_score - top)
    totals = totals * cached_factor + own_factor
    weighted = weighted * cached_factor[..., None] + own_values * own_factor[..., None]
    heads_out = weighted / totals[..., None]
    blended = heads_out[:, :, 0] - map_balance[None, :, None] * heads_out[:, :, 1]
    normed = (
        blended
        * lax.rsqrt(jnp.mean(blended * blended, axis=-1, keepdims=True) + norm_eps)
        * head_gain
    )
    read = normed.reshape(seq_count, HEADS * VD)
    late_rows, read = lax.optimization_barrier((rows, read))
    values = project(late_rows, value_piece)
    key_cache = keys.reshape(1, 1, -1, key_width)
    value_cache = values.reshape(1, 1, -1, value_width)
    return (key_cache, value_cache, read)


def solution(mesh):
    in_specs = (
        P(None, "tp", None, "sp", None, None),
        P(),
        P(None, "tp"),
        P(None, "tp"),
        P(None, "tp"),
        P(),
        P(),
    )
    out_specs = (P("sp", "tp", None, None), P("sp", "tp", None, None), P())
    return jax.shard_map(shards, mesh=mesh, in_specs=in_specs, out_specs=out_specs, check_vma=False)
```

```python
import jax
import jax.numpy as jnp
from jax import lax
from jax.experimental import pallas as pl
from jax.experimental.pallas import tpu as pltpu
from jax.sharding import PartitionSpec as P

HEADS = 8
MAP_HEAD_SIZE = 64
VD = 128


norm_eps = 1e-06


def two_parts(values):
    high = lax.reduce_precision(values, 8, 7)
    return high.astype(jnp.bfloat16), (values - high).astype(jnp.bfloat16)


def project(source, weight):
    return jnp.dot(source, weight, preferred_element_type=jnp.float32).astype(jnp.bfloat16)


def gathered(weight):
    count = lax.axis_size("tp")
    groups = [list(range(core, count, 2)) for core in range(2)]
    return lax.all_gather(weight, "tp", axis=1, tiled=True, axis_index_groups=groups)


def swapped(half):
    count = lax.axis_size("tp")
    return lax.ppermute(half, "tp", [(i, i ^ 1) for i in range(count)])


def project_halves(rows, own, other, width):
    first = (lax.axis_index("tp") % 2 == 0).astype(jnp.int32).reshape(1)
    if width % 128:
        even = jnp.where(first == 1, own, other)
        odd = jnp.where(first == 1, other, own)
        blocks = []
        for start in range(0, own.shape[1], width):
            blocks += [even[:, start : start + width], odd[:, start : start + width]]
        return project(rows, jnp.concatenate(blocks, axis=1))

    def kernel(first_ref, rows_ref, own_ref, other_ref, out_ref):
        is_first = first_ref[0] == 1
        mine, theirs = own_ref[...], other_ref[...]
        pair = jnp.concatenate(
            [jnp.where(is_first, mine, theirs), jnp.where(is_first, theirs, mine)], axis=1
        )
        out_ref[...] = jnp.dot(
            rows_ref[...], pair, preferred_element_type=jnp.float32
        ).astype(out_ref.dtype)

    depth = rows.shape[1]
    count = own.shape[1] // width
    return pl.pallas_call(
        kernel,
        grid=(count,),
        in_specs=[
            pl.BlockSpec(memory_space=pltpu.SMEM),
            pl.BlockSpec(rows.shape, lambda j: (0, 0)),
            pl.BlockSpec((depth, width), lambda j: (0, j)),
            pl.BlockSpec((depth, width), lambda j: (0, j)),
        ],
        out_specs=pl.BlockSpec((rows.shape[0], 2 * width), lambda j: (0, j)),
        out_shape=jax.ShapeDtypeStruct((rows.shape[0], 2 * own.shape[1]), jnp.bfloat16),
        cost_estimate=pl.CostEstimate(
            flops=4 * rows.shape[0] * depth * own.shape[1],
            transcendentals=0,
            bytes_accessed=2 * (rows.size + 2 * own.size + 2 * rows.shape[0] * own.shape[1]),
        ),
        name="project_halves",
    )(first, rows, own, other)


def joined(peak, totals, weighted, axis):
    top = jnp.max(peak, axis=axis, keepdims=True)
    factor = jnp.exp(peak - top)
    return (
        jnp.squeeze(top, axis),
        jnp.sum(totals * factor, axis=axis),
        jnp.sum(weighted * factor[..., None], axis=axis),
    )


def packed(peak, totals, weighted):
    lanes = peak.shape + (VD // 2,)
    return jnp.concatenate(
        [
            weighted,
            jnp.broadcast_to(peak[..., None], lanes),
            jnp.broadcast_to(totals[..., None], lanes),
        ],
        axis=-1,
    )


def unpacked(state):
    width = state.shape[-1] - VD
    return state[..., width], state[..., width + VD // 2], state[..., :width]


def own_read(keys, rows, queries, value_weight):
    tp_count = lax.axis_size("tp")
    map_count = 2 * HEADS
    key_width = keys.shape[1]
    of_map = jnp.arange(key_width) // MAP_HEAD_SIZE == jnp.arange(map_count)[:, None]
    spread = jnp.where(of_map, queries[None, :], jnp.zeros((), queries.dtype))
    scores = lax.dot_general(
        spread, keys, (((1,), (1,)), ((), ())), preferred_element_type=jnp.float32
    ) * MAP_HEAD_SIZE ** (-0.5)
    peak = jnp.max(scores, axis=-1)
    weights_exp = jnp.exp(scores - peak[:, None])
    totals = jnp.sum(weights_exp, axis=-1)
    high, low = two_parts(weights_exp)
    mixed = jnp.dot(
        jnp.concatenate([high, low]), rows, preferred_element_type=jnp.float32
    )
    mixed = mixed[:map_count] + mixed[map_count:]
    state = packed(peak, totals, mixed)
    width = value_weight.shape[1]
    heads_here = max(1, width // VD)
    repeats = max(1, VD // width)
    state = state.reshape(HEADS // heads_here, 1, heads_here * 2, state.shape[-1])
    state = jnp.broadcast_to(state, (state.shape[0], repeats) + state.shape[2:])
    state = state.reshape((tp_count,) + state.shape[2:])
    state = lax.all_to_all(state, "tp", 0, 0, tiled=True)
    peak, totals, mixed = joined(*unpacked(state), 0)
    mixed = mixed.reshape(heads_here, 2, -1)
    head_weight = value_weight.reshape(value_weight.shape[0], heads_here, width // heads_here)
    high, low = two_parts(mixed)
    weighted = jnp.einsum(
        "hmd,dhe->hme",
        jnp.concatenate([high, low], axis=1),
        head_weight,
        preferred_element_type=jnp.float32,
    )
    weighted = weighted[:, :2] + weighted[:, 2:]
    return peak, totals, weighted.reshape(heads_here * 2, -1)


def shards(prompt, new_token, query_proj_matrix, key_weight, value_weight, map_balance, head_gain):
    seq_count, _, span_count, _, piece_rows, model_width = prompt.shape
    tp_count = lax.axis_size("tp")
    slot_count = seq_count * span_count
    key_width = key_weight.shape[1] * tp_count
    value_width = value_weight.shape[1] * tp_count
    key_half = gathered(key_weight)
    value_half = gathered(value_weight)
    rows = lax.all_to_all(
        prompt.reshape(slot_count, piece_rows, model_width),
        "sp",
        split_axis=0,
        concat_axis=1,
        tiled=True,
    )
    rows = rows.reshape(-1, model_width)
    own_columns = jnp.stack(
        [project(new_token, w) for w in (query_proj_matrix, key_weight, value_weight)]
    )
    queries, new_keys, new_values = lax.all_gather(own_columns, "tp", axis=2, tiled=True)
    key_half, rows, queries = lax.optimization_barrier((key_half, rows, queries))
    keys = project_halves(rows, key_half, swapped(key_half), key_weight.shape[1])
    own_seq = lax.axis_index("sp") // span_count
    peak, totals, weighted = own_read(
        keys, rows, lax.dynamic_index_in_dim(queries, own_seq, 0, False), value_weight
    )
    state = lax.all_gather(packed(peak, totals, weighted), "sp")
    state = state.reshape((seq_count, span_count) + state.shape[1:])
    peak, totals, weighted = joined(*unpacked(state), 1)
    state = packed(peak, totals, weighted)
    value_half, state = lax.optimization_barrier((value_half, state))
    other_values = swapped(value_half)
    state = lax.all_gather(state, "tp")
    peak, totals, weighted = unpacked(state)
    heads_here = weighted.shape[2] // 2
    groups = HEADS // heads_here
    repeats = tp_count // groups
    peak, totals = (
        jnp.swapaxes(
            a.reshape(groups, repeats, seq_count, heads_here, 2)[:, 0], 0, 1
        ).reshape(seq_count, HEADS, 2)
        for a in (peak, totals)
    )
    weighted = weighted.reshape(groups, repeats, seq_count, heads_here, 2, -1)
    weighted = jnp.transpose(weighted, (2, 0, 3, 4, 1, 5)).reshape(seq_count, HEADS, 2, VD)
    own_score = jnp.sum(
        (queries.astype(jnp.float32) * new_keys.astype(jnp.float32)).reshape(
            seq_count, HEADS, 2, MAP_HEAD_SIZE
        ),
        axis=-1,
    ) * MAP_HEAD_SIZE ** (-0.5)
    own_values = new_values.astype(jnp.float32).reshape(seq_count, HEADS, 1, VD)
    top = jnp.maximum(peak, own_score)
    cached_factor = jnp.exp(peak - top)
    own_factor = jnp.exp(own_score - top)
    totals = totals * cached_factor + own_factor
    weighted = weighted * cached_factor[..., None] + own_values * own_factor[..., None]
    heads_out = weighted / totals[..., None]
    blended = heads_out[:, :, 0] - map_balance[None, :, None] * heads_out[:, :, 1]
    normed = (
        blended
        * lax.rsqrt(jnp.mean(blended * blended, axis=-1, keepdims=True) + norm_eps)
        * head_gain
    )
    read = normed.reshape(seq_count, HEADS * VD)
    late_rows, read = lax.optimization_barrier((rows, read))
    values = project_halves(late_rows, value_half, other_values, value_weight.shape[1])
    key_cache = keys.reshape(1, 1, -1, key_width)
    value_cache = values.reshape(1, 1, -1, value_width)
    return (key_cache, value_cache, read)


def solution(mesh):
    in_specs = (
        P(None, "tp", None, "sp", None, None),
        P(),
        P(None, "tp"),
        P(None, "tp"),
        P(None, "tp"),
        P(),
        P(),
    )
    out_specs = (P("sp", "tp", None, None), P("sp", "tp", None, None), P())
    return jax.shard_map(shards, mesh=mesh, in_specs=in_specs, out_specs=out_specs, check_vma=False)
```

```python
import jax
import jax.numpy as jnp
from jax import lax
from jax.experimental import pallas as pl
from jax.sharding import PartitionSpec as P

HEADS = 8
MAP_HEAD_SIZE = 64
VD = 128


norm_eps = 1e-06


def two_parts(values):
    high = lax.reduce_precision(values, 8, 7)
    return high.astype(jnp.bfloat16), (values - high).astype(jnp.bfloat16)


def project(source, weight):
    return jnp.dot(source, weight, preferred_element_type=jnp.float32).astype(jnp.bfloat16)


def gathered(weight):
    count = lax.axis_size("sp")
    part = weight.shape[0] // count
    own = lax.dynamic_slice_in_dim(weight, lax.axis_index("sp") * part, part, 0)
    whole = lax.all_gather(own, ("sp", "tp"), axis=0, tiled=True)
    return whole.reshape(count, lax.axis_size("tp"), part, weight.shape[1])


def project_blocks(rows, blocks):
    parts, count, part, width = blocks.shape
    depth = parts * part
    if width % 128 or count % 2:
        weight = jnp.transpose(blocks, (0, 2, 1, 3)).reshape(depth, count * width)
        return project(rows, weight)

    def kernel(rows_ref, block_ref, out_ref):
        pair = jnp.concatenate(
            [block_ref[:, side].reshape(depth, width) for side in range(2)], axis=1
        )
        out_ref[...] = jnp.dot(
            rows_ref[...], pair, preferred_element_type=jnp.float32
        ).astype(out_ref.dtype)

    return pl.pallas_call(
        kernel,
        grid=(count // 2,),
        in_specs=[
            pl.BlockSpec(rows.shape, lambda j: (0, 0)),
            pl.BlockSpec((parts, 2, part, width), lambda j: (0, j, 0, 0)),
        ],
        out_specs=pl.BlockSpec((rows.shape[0], 2 * width), lambda j: (0, j)),
        out_shape=jax.ShapeDtypeStruct((rows.shape[0], count * width), jnp.bfloat16),
        cost_estimate=pl.CostEstimate(
            flops=2 * rows.shape[0] * blocks.size,
            transcendentals=0,
            bytes_accessed=2 * (rows.size + blocks.size + rows.shape[0] * count * width),
        ),
        name="project_blocks",
    )(rows, blocks)


def joined(peak, totals, weighted, axis):
    top = jnp.max(peak, axis=axis, keepdims=True)
    factor = jnp.exp(peak - top)
    return (
        jnp.squeeze(top, axis),
        jnp.sum(totals * factor, axis=axis),
        jnp.sum(weighted * factor[..., None], axis=axis),
    )


def packed(peak, totals, weighted):
    lanes = peak.shape + (VD // 2,)
    return jnp.concatenate(
        [
            weighted,
            jnp.broadcast_to(peak[..., None], lanes),
            jnp.broadcast_to(totals[..., None], lanes),
        ],
        axis=-1,
    )


def unpacked(state):
    width = state.shape[-1] - VD
    return state[..., width], state[..., width + VD // 2], state[..., :width]


def own_read(keys, rows, queries, value_weight):
    tp_count = lax.axis_size("tp")
    map_count = 2 * HEADS
    key_width = keys.shape[1]
    of_map = jnp.arange(key_width) // MAP_HEAD_SIZE == jnp.arange(map_count)[:, None]
    spread = jnp.where(of_map, queries[None, :], jnp.zeros((), queries.dtype))
    scores = lax.dot_general(
        spread, keys, (((1,), (1,)), ((), ())), preferred_element_type=jnp.float32
    ) * MAP_HEAD_SIZE ** (-0.5)
    peak = jnp.max(scores, axis=-1)
    weights_exp = jnp.exp(scores - peak[:, None])
    totals = jnp.sum(weights_exp, axis=-1)
    high, low = two_parts(weights_exp)
    mixed = jnp.dot(
        jnp.concatenate([high, low]), rows, preferred_element_type=jnp.float32
    )
    mixed = mixed[:map_count] + mixed[map_count:]
    state = packed(peak, totals, mixed)
    width = value_weight.shape[1]
    heads_here = max(1, width // VD)
    repeats = max(1, VD // width)
    state = state.reshape(HEADS // heads_here, 1, heads_here * 2, state.shape[-1])
    state = jnp.broadcast_to(state, (state.shape[0], repeats) + state.shape[2:])
    state = state.reshape((tp_count,) + state.shape[2:])
    state = lax.all_to_all(state, "tp", 0, 0, tiled=True)
    peak, totals, mixed = joined(*unpacked(state), 0)
    mixed = mixed.reshape(heads_here, 2, -1)
    head_weight = value_weight.reshape(value_weight.shape[0], heads_here, width // heads_here)
    high, low = two_parts(mixed)
    weighted = jnp.einsum(
        "hmd,dhe->hme",
        jnp.concatenate([high, low], axis=1),
        head_weight,
        preferred_element_type=jnp.float32,
    )
    weighted = weighted[:, :2] + weighted[:, 2:]
    return peak, totals, weighted.reshape(heads_here * 2, -1)


def shards(prompt, new_token, query_proj_matrix, key_weight, value_weight, map_balance, head_gain):
    seq_count, _, span_count, _, piece_rows, model_width = prompt.shape
    tp_count = lax.axis_size("tp")
    slot_count = seq_count * span_count
    key_width = key_weight.shape[1] * tp_count
    value_width = value_weight.shape[1] * tp_count
    key_blocks = gathered(key_weight)
    value_blocks = gathered(value_weight)
    rows = lax.all_to_all(
        prompt.reshape(slot_count, piece_rows, model_width),
        "sp",
        split_axis=0,
        concat_axis=1,
        tiled=True,
    )
    rows = rows.reshape(-1, model_width)
    own_columns = jnp.stack(
        [project(new_token, w) for w in (query_proj_matrix, key_weight, value_weight)]
    )
    queries, new_keys, new_values = lax.all_gather(own_columns, "tp", axis=2, tiled=True)
    keys = project_blocks(rows, key_blocks)
    own_seq = lax.axis_index("sp") // span_count
    peak, totals, weighted = own_read(
        keys, rows, lax.dynamic_index_in_dim(queries, own_seq, 0, False), value_weight
    )
    state = lax.all_gather(packed(peak, totals, weighted), "sp")
    state = state.reshape((seq_count, span_count) + state.shape[1:])
    peak, totals, weighted = joined(*unpacked(state), 1)
    state = packed(peak, totals, weighted)
    late_rows, state = lax.optimization_barrier((rows, state))
    state = lax.all_to_all(
        jnp.broadcast_to(state[None], (tp_count,) + state.shape), "tp", 0, 0, tiled=True
    )
    peak, totals, weighted = unpacked(state)
    heads_here = weighted.shape[2] // 2
    groups = HEADS // heads_here
    repeats = tp_count // groups
    peak, totals = (
        jnp.swapaxes(
            a.reshape(groups, repeats, seq_count, heads_here, 2)[:, 0], 0, 1
        ).reshape(seq_count, HEADS, 2)
        for a in (peak, totals)
    )
    weighted = weighted.reshape(groups, repeats, seq_count, heads_here, 2, -1)
    weighted = jnp.transpose(weighted, (2, 0, 3, 4, 1, 5)).reshape(seq_count, HEADS, 2, VD)
    own_score = jnp.sum(
        (queries.astype(jnp.float32) * new_keys.astype(jnp.float32)).reshape(
            seq_count, HEADS, 2, MAP_HEAD_SIZE
        ),
        axis=-1,
    ) * MAP_HEAD_SIZE ** (-0.5)
    own_values = new_values.astype(jnp.float32).reshape(seq_count, HEADS, 1, VD)
    top = jnp.maximum(peak, own_score)
    cached_factor = jnp.exp(peak - top)
    own_factor = jnp.exp(own_score - top)
    totals = totals * cached_factor + own_factor
    weighted = weighted * cached_factor[..., None] + own_values * own_factor[..., None]
    heads_out = weighted / totals[..., None]
    blended = heads_out[:, :, 0] - map_balance[None, :, None] * heads_out[:, :, 1]
    normed = (
        blended
        * lax.rsqrt(jnp.mean(blended * blended, axis=-1, keepdims=True) + norm_eps)
        * head_gain
    )
    read = normed.reshape(seq_count, HEADS * VD)
    values = project_blocks(late_rows, value_blocks)
    key_cache = keys.reshape(1, 1, -1, key_width)
    value_cache = values.reshape(1, 1, -1, value_width)
    return (key_cache, value_cache, read)


def solution(mesh):
    in_specs = (
        P(None, "tp", None, "sp", None, None),
        P(),
        P(None, "tp"),
        P(None, "tp"),
        P(None, "tp"),
        P(),
        P(),
    )
    out_specs = (P("sp", "tp", None, None), P("sp", "tp", None, None), P())
    return jax.shard_map(shards, mesh=mesh, in_specs=in_specs, out_specs=out_specs, check_vma=False)
```
